32 devices in a mesh: sp: 8 (over z, x), tp: 4 (over y, core).
Axes of the slice: x: 2, y: 2, z: 4, core: 2. Of those that a mesh axis runs over, the one named last changes fastest.
Arguments:
- stream: bfloat16 [2048, 2048], P(('sp', 'tp')), may hold values from -6 to 6
- query_a: bfloat16 [2048, 384], P('sp', 'tp'), may hold values from -400 to 400
- query_b: bfloat16 [2048, 640], P('sp', 'tp'), may hold values from -400 to 400
- latent: bfloat16 [2048, 256], P('sp'), may hold values from -6 to 6
- rotary_key: bfloat16 [2048, 32], P('sp'), may hold values from -6 to 6
- latent_gain: float32 [256], replicated, may hold values from 0.1 to 1.9
- key_gain_a: float32 [96], replicated, may hold values from 0.1 to 1.9
- key_gain_b: float32 [160], replicated, may hold values from 0.1 to 1.9
- w_key_a: bfloat16 [256, 256], P(None, 'tp'), may hold values from -0.375 to 0.375
- w_value_a: bfloat16 [256, 256], P(None, 'tp'), may hold values from -0.375 to 0.375
- w_key_b: bfloat16 [256, 512], P(None, 'tp'), may hold values from -0.375 to 0.375
- w_value_b: bfloat16 [256, 512], P(None, 'tp'), may hold values from -0.375 to 0.375
- w_out_a: bfloat16 [256, 2048], P('tp'), may hold values from -0.21875 to 0.21875
- w_out_b: bfloat16 [512, 2048], P('tp'), may hold values from -0.21875 to 0.21875
- norm_gain: float32 [2048], replicated, may hold values from 0.1 to 1.9
- w_up: bfloat16 [2048, 4096], P('sp', 'tp'), may hold values from -0.125 to 0.125
- w_down: bfloat16 [4096, 2048], P('tp', 'sp'), may hold values from -0.09375 to 0.09375
Outputs:
- result: bfloat16 [2048, 2048], P(('sp', 'tp'))
The draws below stay inside these ranges and needn't reach their ends.
All inputs are finite; a program needn't handle non-finite values.
Results may differ from the reference program's by a relative error of at most 0.018.
The reference program's roundings to bfloat16 on the way count: a program that leaves them out, or rounds other values in their place, can miss the bound.
Values may be sent and summed in bfloat16 or wider, within the bound.
A program may use at most 128 MiB of HBM per device.

```python
import math
import jax
import jax.numpy as jnp
from jax import lax

D = 2048
HEADS_A = 4
HEADS_B = 4
NOPE_A = 64
V_A = 64
NOPE_B = 128
V_B = 128
ROPE = 32
KV_RANK = 256
FF = 4096
TOKENS = 2048


def scaled_rows(key, count, width):
    base_key = jax.random.fold_in(key, 0)
    base = jax.random.normal(base_key, (count, width), jnp.float32)
    factor = 2.5 * jnp.ones((count, 1), jnp.float32)
    return jnp.clip(base * factor, -400.0, 400.0)


def draw_query_a(key, part):
    return scaled_rows(jax.random.fold_in(key, 11), TOKENS, HEADS_A * (NOPE_A + ROPE)).astype(jnp.bfloat16)


def draw_query_b(key, part):
    return scaled_rows(jax.random.fold_in(key, 23), TOKENS, HEADS_B * (NOPE_B + ROPE)).astype(jnp.bfloat16)


def block_scale(stream_key, shape, shards, smallest, largest):
    level = 1.0
    for position, blocks in shards:
        heights = jax.random.uniform(jax.random.fold_in(jax.random.fold_in(stream_key, 6), position), (blocks,), jnp.float32, smallest / len(shards), largest / len(shards))
        level = level * jnp.repeat(jnp.exp(heights), shape[position] // blocks).reshape((-1,) + (1,) * (len(shape) - 1 - position))
    return level


def scatter_about(own_key, shape, scale, reach, cuts=(), kind=jnp.bfloat16):
    array = scale * jax.random.normal(own_key, shape, jnp.float32)
    if cuts:
        array = array * block_scale(own_key, shape, cuts, -0.22, 0.18)
    return jnp.clip(array, -reach, reach).astype(kind)


def setup_inputs(seed: int = 0) -> dict:
    splits = jax.random.split(jax.random.key(seed), 18)
    stream = scatter_about(splits[0], (TOKENS, D), 0.4, 6.0, ((0, 32),))
    query_a = draw_query_a(jax.random.fold_in(splits[17], 71), 0)
    query_b = draw_query_b(jax.random.fold_in(splits[17], 71), 0)
    latent = scatter_about(splits[3], (TOKENS, KV_RANK), 1.0, 6.0, ((0, 8),))
    rotary_key = scatter_about(splits[4], (TOKENS, ROPE), 1.0, 6.0, ((0, 8),))
    latent_gain = jnp.clip(1.0 + 0.18 * jax.random.normal(splits[5], (KV_RANK,), jnp.float32), 0.1, 1.9)
    key_gain_a = jnp.clip(1.0 + 0.18 * jax.random.normal(splits[6], (NOPE_A + ROPE,), jnp.float32), 0.1, 1.9)
    key_gain_b = jnp.clip(1.0 + 0.18 * jax.random.normal(splits[7], (NOPE_B + ROPE,), jnp.float32), 0.1, 1.9)
    w_key_a = scatter_about(splits[8], (KV_RANK, HEADS_A * NOPE_A), KV_RANK ** -0.5, 0.375, ((1, 4),))
    w_value_a = scatter_about(splits[9], (KV_RANK, HEADS_A * V_A), KV_RANK ** -0.5, 0.375, ((1, 4),))
    w_key_b = scatter_about(splits[10], (KV_RANK, HEADS_B * NOPE_B), KV_RANK ** -0.5, 0.375, ((1, 4),))
    w_value_b = scatter_about(splits[11], (KV_RANK, HEADS_B * V_B), KV_RANK ** -0.5, 0.375, ((1, 4),))
    w_out_a = scatter_about(splits[12], (HEADS_A * V_A, D), (HEADS_A * V_A + HEADS_B * V_B) ** -0.5, 0.21875, ((0, 4),))
    w_out_b = scatter_about(splits[13], (HEADS_B * V_B, D), (HEADS_A * V_A + HEADS_B * V_B) ** -0.5, 0.21875, ((0, 4),))
    norm_gain = jnp.clip(1.0 + 0.18 * jax.random.normal(splits[14], (D,), jnp.float32), 0.1, 1.9)
    w_up = scatter_about(splits[15], (D, FF), D ** -0.5, 0.125, ((0, 8), (1, 4)))
    w_down = scatter_about(splits[16], (FF, D), FF ** -0.5, 0.09375, ((0, 4), (1, 8)))
    return {"stream": stream, "query_a": query_a, "query_b": query_b, "latent": latent, "rotary_key": rotary_key, "latent_gain": latent_gain, "key_gain_a": key_gain_a, "key_gain_b": key_gain_b, "w_key_a": w_key_a, "w_value_a": w_value_a, "w_key_b": w_key_b, "w_value_b": w_value_b, "w_out_a": w_out_a, "w_out_b": w_out_b, "norm_gain": norm_gain, "w_up": w_up, "w_down": w_down}


EPSILON = 1e-06
THETA = 10000.0

def rms_scale(values, gain):
    wide = values.astype(jnp.float32)
    return wide * lax.rsqrt(lax.optimization_barrier(jnp.mean(wide * wide, axis=-1, keepdims=True)) + EPSILON) * gain.astype(jnp.float32)

def rotate(tail, positions):
    half = tail.shape[-1] // 2
    freqs = THETA ** (-jnp.arange(half, dtype=jnp.float32) / half)
    angle = positions[:, None, None] * freqs
    cosine = jnp.cos(angle)
    sine = jnp.sin(angle)
    first = tail[..., :half]
    second = tail[..., half:]
    return jnp.concatenate([first * cosine - second * sine, second * cosine + first * sine], axis=-1)

def make_keys(normed, rotary_key, w_key, w_value, key_gain, nope, positions):
    count = normed.shape[0]
    heads = w_key.shape[1] // nope
    head_nope = jnp.dot(normed, w_key, preferred_element_type=jnp.float32).astype(jnp.bfloat16)
    head_nope = head_nope.reshape(count, heads, nope)
    values = jnp.dot(normed, w_value, preferred_element_type=jnp.float32).astype(jnp.bfloat16)
    shared = jnp.broadcast_to(rotary_key[:, None, :], (count, heads, rotary_key.shape[1]))
    joined = rms_scale(jnp.concatenate([head_nope, shared], axis=-1), key_gain)
    turned = rotate(joined[..., nope:], positions)
    keys_out = jnp.concatenate([joined[..., :nope], turned], axis=-1).astype(jnp.bfloat16)
    return (keys_out.reshape(count, -1), values)

def attention(queries, keys_in, values_in, depth):
    total_rows = keys_in.shape[0]
    heads = keys_in.shape[1] // depth
    key_view = keys_in.astype(jnp.float32).reshape(total_rows, heads, depth)
    value_view = values_in.astype(jnp.float32).reshape(total_rows, heads, -1)
    block = math.gcd(queries.shape[0], 512)
    blocks = queries.astype(jnp.float32).reshape(-1, block, heads, depth)

    def one_block(block_queries):
        scores = jnp.einsum('qhd,khd->qhk', block_queries, key_view) * depth ** (-0.5)
        peak = lax.optimization_barrier(jnp.max(scores, axis=-1))
        shifted = jnp.exp(scores - peak[..., None])
        totals = lax.optimization_barrier(jnp.sum(shifted, axis=-1))
        weights = lax.optimization_barrier(shifted.astype(jnp.bfloat16)).astype(jnp.float32)
        weighted = jnp.einsum('qhk,khd->qhd', weights, value_view)
        return (weighted / totals[..., None]).astype(jnp.bfloat16).reshape(block, -1)
    return lax.map(one_block, blocks).reshape(queries.shape[0], -1)

def reference(stream, query_a, query_b, latent, rotary_key, latent_gain, key_gain_a, key_gain_b, w_key_a, w_value_a, w_key_b, w_value_b, w_out_a, w_out_b, norm_gain, w_up, w_down):
    positions = jnp.arange(TOKENS).astype(jnp.float32)
    normed_latent = rms_scale(latent, latent_gain).astype(jnp.bfloat16)
    key_a, value_a = make_keys(normed_latent, rotary_key, w_key_a, w_value_a, key_gain_a, NOPE_A, positions)
    key_b, value_b = make_keys(normed_latent, rotary_key, w_key_b, w_value_b, key_gain_b, NOPE_B, positions)
    attended_a = attention(query_a, key_a, value_a, NOPE_A + ROPE)
    attended_b = attention(query_b, key_b, value_b, NOPE_B + ROPE)
    mixed = jnp.dot(attended_a, w_out_a, preferred_element_type=jnp.float32) + jnp.dot(attended_b, w_out_b, preferred_element_type=jnp.float32)
    residual = (stream.astype(jnp.float32) + mixed).astype(jnp.bfloat16)
    normed = rms_scale(residual, norm_gain).astype(jnp.bfloat16)
    activated = jnp.square(jax.nn.relu(jnp.dot(normed, w_up, preferred_element_type=jnp.float32))).astype(jnp.bfloat16)
    summed = jnp.dot(activated, w_down, preferred_element_type=jnp.float32)
    return (residual.astype(jnp.float32) + summed).astype(jnp.bfloat16)
```

```python
import functools

import jax
import jax.numpy as jnp
from jax import lax
from jax.experimental import pallas as pl
from jax.experimental.pallas import tpu as pltpu
from jax.sharding import PartitionSpec as P

NOPE_A = 64
V_A = 64
NOPE_B = 128
V_B = 128
ROPE = 32

EPSILON = 1e-06
THETA = 10000.0
F32 = jnp.float32
BF16 = jnp.bfloat16


def kernel(
    n, m,
    stream, q_a, q_b, packed, table, lat_gain, gain_a, gain_b,
    wk_a, wv_a, wk_b, wv_b, wo_a, wo_b, norm_gain, w_up, w_down,
    out,
    lat, key_a, key_b, val_a, val_b, att, rows, goa, gob,
    gup, gdown, x, hid, act, res, even, odd, sib, mid, part, land,
    lat_s, lat_r, latf_s, latf_r, oa_s, oa_r, ob_s, ob_r,
    up_s, up_r, dn_s, dn_r, at_s, at_r, x_s, x_r, rs_s, rs_r,
):
    s = lax.axis_index("sp")
    t = lax.axis_index("tp")
    core = t & 1
    length = q_a.shape[0]
    own = stream.shape[0]
    prow = packed.shape[0]
    half_rows = prow // 2
    depth_a = NOPE_A + ROPE
    depth_b = NOPE_B + ROPE
    heads_a = wk_a.shape[1] // NOPE_A
    heads_b = wk_b.shape[1] // NOPE_B
    hidden = gup.shape[2]
    wrows = w_up.shape[0]
    wcols = w_down.shape[1]
    width_a = heads_a * V_A
    width_b = heads_b * V_B
    start_b = att.shape[2] - width_b
    pending = []

    def copy(src, dst, ssem, rsem, sp, tp):
        return pltpu.make_async_remote_copy(
            src_ref=src, dst_ref=dst, send_sem=ssem, recv_sem=rsem,
            device_id={"sp": sp, "tp": tp}, device_id_type=pl.DeviceIdType.MESH,
        )

    def send(*args):
        c = copy(*args)
        c.start()
        pending.append(c)

    barrier = pltpu.get_barrier_semaphore()
    for k in range(1, n):
        pl.semaphore_signal(barrier, inc=1, device_id={"sp": s ^ k, "tp": t},
                            device_id_type=pl.DeviceIdType.MESH)
    for k in range(1, m):
        pl.semaphore_signal(barrier, inc=1, device_id={"sp": s, "tp": t ^ k},
                            device_id_type=pl.DeviceIdType.MESH)
    pl.semaphore_wait(barrier, n + m - 2)

    mine = pl.ds(pl.multiple_of(core * half_rows, 16), half_rows)
    other = pl.ds(pl.multiple_of((1 - core) * half_rows, 16), half_rows)
    for k in range(1, n):
        send(packed.at[mine], lat.at[k, mine], lat_s.at[k], lat_r.at[k], s ^ k, t)
    for k in (2, 1):
        send(wo_a, goa.at[k - 1], oa_s.at[k - 1], oa_r.at[k - 1], s, t ^ k)
        send(wo_b, gob.at[k - 1], ob_s.at[k - 1], ob_r.at[k - 1], s, t ^ k)

    def halves(target):
        return pl.ds(pl.multiple_of(((target // 2) % 2) * hidden, 128), hidden)

    for k in [1] + list(range(2, n, 2)):
        send(w_up.at[:, halves(s ^ k)], gup.at[k], up_s.at[k], up_r.at[k], s ^ k, t)
    for k in [1] + list(range(2, n, 2)):
        send(w_down.at[halves(s ^ k)], gdown.at[k], dn_s.at[k], dn_r.at[k], s ^ k, t)

    def make_block(k, source):
        start = pl.multiple_of(k * length, length)
        at = pl.ds(start, length)
        wide = source[0:length, :].astype(F32)
        normed = (wide * lax.rsqrt(jnp.mean(wide * wide, axis=-1, keepdims=True) + EPSILON)
                  * lat_gain[...]).astype(BF16)
        tail = source[length:prow, :].astype(F32)
        lanes = tail.shape[1] // ROPE
        rotary = jnp.concatenate([tail[:, i * ROPE:(i + 1) * ROPE] for i in range(lanes)], axis=0)
        squares = jnp.sum(rotary * rotary, axis=-1, keepdims=True)
        turn = table[s ^ k]
        half = ROPE // 2

        def keys(wk, gain, nope, heads, dest):
            flat = jnp.dot(normed, wk[...], preferred_element_type=F32).astype(BF16).astype(F32)
            for h in range(heads):
                piece = flat[:, h * nope:(h + 1) * nope]
                mean = (jnp.sum(piece * piece, axis=-1, keepdims=True) + squares) / (nope + ROPE)
                scale = lax.rsqrt(mean + EPSILON)
                dest[h, at, 0:nope] = (piece * scale * gain[:, 0:nope]).astype(BF16)
                last = rotary * scale * gain[:, nope:nope + ROPE]
                swapped = jnp.concatenate([last[:, half:], last[:, :half]], axis=-1)
                dest[h, at, nope:nope + ROPE] = (
                    last * turn[:, 0:ROPE] + swapped * turn[:, ROPE:2 * ROPE]).astype(BF16)

        keys(wk_a, gain_a, NOPE_A, heads_a, key_a)
        keys(wk_b, gain_b, NOPE_B, heads_b, key_b)
        val_a[at, :] = jnp.dot(normed, wv_a[...], preferred_element_type=F32).astype(BF16)
        val_b[at, :] = jnp.dot(normed, wv_b[...], preferred_element_type=F32).astype(BF16)

    make_block(0, packed)
    for k in range(1, n):
        copy(packed.at[mine], lat.at[k, mine], lat_s.at[k], lat_r.at[k], s ^ k, t).wait_recv()
        send(lat.at[k, mine], lat.at[k, mine], latf_s.at[k], latf_r.at[k], s, t ^ 1)
    copy(wo_a, goa.at[1], oa_s.at[1], oa_r.at[1], s, t ^ 2).wait_recv()
    send(goa.at[1], goa.at[2], oa_s.at[2], oa_r.at[2], s, t ^ 1)
    copy(wo_b, gob.at[1], ob_s.at[1], ob_r.at[1], s, t ^ 2).wait_recv()
    send(gob.at[1], gob.at[2], ob_s.at[2], ob_r.at[2], s, t ^ 1)

    def one(k, carry):
        copy(lat.at[k, other], lat.at[k, other], latf_s.at[k], latf_r.at[k], s, t ^ 1).wait_recv()
        make_block(k, lat.at[k])
        return carry

    lax.fori_loop(1, n, one, 0)

    total = n * length
    block = min(total, 2048)
    number = total // block

    def attend(q, key, value, h, depth, width):
        query = q[:, h * depth:(h + 1) * depth]

        def step(i, state):
            peak, sums, acc = state
            at = pl.ds(pl.multiple_of(i * block, block), block)
            score = lax.dot_general(query, key[h, at, :], (((1,), (1,)), ((), ())),
                                    preferred_element_type=F32) * depth ** (-0.5)
            new = jnp.maximum(peak, jnp.max(score, axis=-1, keepdims=True))
            shifted = jnp.exp(score - new)
            factor = jnp.exp(peak - new)
            sums = sums * factor + jnp.sum(shifted, axis=-1, keepdims=True)
            acc = acc * factor + jnp.dot(
                shifted.astype(BF16), value[at, h * width:(h + 1) * width],
                preferred_element_type=F32)
            return new, sums, acc

        state = (jnp.full((length, 1), -jnp.inf, F32), jnp.zeros((length, 1), F32),
                 jnp.zeros((length, width), F32))
        if number == 1:
            state = step(0, state)
        else:
            state = lax.fori_loop(0, number, step, state)
        return (state[2] / state[1]).astype(BF16)

    for h in range(heads_a):
        res_a = attend(q_a, key_a, val_a, h, depth_a, V_A)
        for j in range(m):
            att[j, :, h * V_A:(h + 1) * V_A] = res_a[j * own:(j + 1) * own]
    for h in range(heads_b):
        res_b = attend(q_b, key_b, val_b, h, depth_b, V_B)
        for j in range(m):
            att[j, :, start_b + h * V_B:start_b + (h + 1) * V_B] = res_b[j * own:(j + 1) * own]
    for k in range(1, m):
        send(att.at[t ^ k], rows.at[k], at_s.at[k], at_r.at[k], s, t ^ k)

    for k in range(2, n, 2):
        copy(gup.at[k], gup.at[k], up_s.at[k], up_r.at[k], s ^ k, t).wait_recv()
        send(gup.at[k], gup.at[k + 1], up_s.at[k + 1], up_r.at[k + 1], s ^ 1, t)

    mixed = (jnp.dot(att[t, :, 0:width_a], wo_a[...], preferred_element_type=F32)
             + jnp.dot(att[t, :, start_b:], wo_b[...], preferred_element_type=F32))
    for k in range(1, m):
        copy(wo_a, goa.at[k - 1], oa_s.at[k - 1], oa_r.at[k - 1], s, t ^ 1) \
            .wait_recv() if k != 2 else None
        copy(wo_b, gob.at[k - 1], ob_s.at[k - 1], ob_r.at[k - 1], s, t ^ 1) \
            .wait_recv() if k != 2 else None
        copy(att.at[t ^ k], rows.at[k], at_s.at[k], at_r.at[k], s, t ^ k).wait_recv()
        mixed += jnp.dot(rows[k, :, 0:width_a], goa[k - 1], preferred_element_type=F32)
        mixed += jnp.dot(rows[k, :, start_b:], gob[k - 1], preferred_element_type=F32)
    residual = (stream[...].astype(F32) + mixed).astype(BF16)
    res[...] = residual
    wide = residual.astype(F32)
    x[0:own, :] = (wide * lax.rsqrt(jnp.mean(wide * wide, axis=-1, keepdims=True) + EPSILON)
                   * norm_gain[...]).astype(BF16)

    def peer(code):
        return (s ^ 2 if code & 4 else s), t ^ (code & 3)

    def slot(k):
        return x.at[pl.ds(k * own, own)]

    def xcopy(src, dst, code):
        return copy(slot(src), slot(dst), x_s.at[dst], x_r.at[dst], *peer(code))

    def xsend(src, dst, code):
        c = xcopy(src, dst, code)
        c.start()
        pending.append(c)

    for code in (2, 4, 1):
        xsend(0, code, code)
    xcopy(0, 2, 2).wait_recv()
    xcopy(0, 4, 4).wait_recv()
    diag = copy(
        x.at[pl.ds(pl.multiple_of((2 + 2 * core) * own, own), own)], slot(6),
        x_s.at[6], x_r.at[6], s ^ (2 - 2 * core), t ^ (2 * core))
    diag.start()
    pending.append(diag)
    xsend(2, 3, 1)
    xsend(4, 5, 1)
    diag.wait_recv()
    xsend(6, 7, 1)
    for k in range(2, n, 2):
        copy(gdown.at[k], gdown.at[k], dn_s.at[k], dn_r.at[k], s ^ k, t).wait_recv()
        send(gdown.at[k], gdown.at[k + 1], dn_s.at[k + 1], dn_r.at[k + 1], s ^ 1, t)
    for k in (1, 3, 5, 7):
        xcopy(k - 1, k, 1).wait_recv()

    def columns(k, size):
        return pl.ds(pl.multiple_of((s ^ k) * size, 128), size)

    held = halves(s)
    hid[...] = jnp.dot(x[:, columns(0, wrows)], w_up[:, held], preferred_element_type=F32)
    for k in [1] + list(range(3, n, 2)):
        copy(gup.at[k], gup.at[k], up_s.at[k], up_r.at[k], s ^ 1, t).wait_recv()

    def up(k, carry):
        hid[...] += jnp.dot(x[:, columns(k, wrows)], gup[k], preferred_element_type=F32)
        return carry

    lax.fori_loop(1, n, up, 0)
    act[...] = jnp.square(jnp.maximum(hid[...], 0.0)).astype(BF16)
    for k in [1] + list(range(3, n, 2)):
        copy(gdown.at[k], gdown.at[k], dn_s.at[k], dn_r.at[k], s ^ 1, t).wait_recv()

    def split(k, piece):
        at = columns(k, wcols)
        for i in range(4):
            even[i, :, at] = piece[2 * i * own:(2 * i + 1) * own]
            odd[i, :, at] = piece[(2 * i + 1) * own:(2 * i + 2) * own].astype(BF16)

    split(0, jnp.dot(act[...], w_down[held, :], preferred_element_type=F32))

    def down(k, carry):
        split(k, jnp.dot(act[...], gdown[k], preferred_element_type=F32))
        return carry

    lax.fori_loop(1, n, down, 0)

    first = copy(odd, sib, rs_s.at[0], rs_r.at[0], s, t ^ 1)
    first.start()
    pending.append(first)
    first.wait_recv()
    mid[...] = (even[3] + sib[3].astype(F32)).astype(BF16)
    second = copy(mid, land.at[0], rs_s.at[1], rs_r.at[1], s ^ (2 - 2 * core), t ^ (2 * core))
    second.start()
    pending.append(second)
    for i in range(3):
        even[i] += sib[i].astype(F32)
    second.wait_recv()
    even[1 + core] += land[0].astype(F32)
    for i in (1, 2):
        part[i - 1] = even[i].astype(BF16)
    third = copy(part.at[0], land.at[1], rs_s.at[2], rs_r.at[2], s, t ^ 2)
    third.start()
    fourth = copy(part.at[1], land.at[2], rs_s.at[3], rs_r.at[3], s ^ 2, t)
    fourth.start()
    pending.append(third)
    pending.append(fourth)
    third.wait_recv()
    fourth.wait_recv()
    summed = even[0] + land[1].astype(F32) + land[2].astype(F32)
    out[...] = (res[...].astype(F32) + summed).astype(BF16)
    for c in pending:
        c.wait_send()


def body(n, m, stream, query_a, query_b, latent, rotary_key, latent_gain, key_gain_a, key_gain_b,
         w_key_a, w_value_a, w_key_b, w_value_b, w_out_a, w_out_b, norm_gain, w_up, w_down):
    length, rank = latent.shape
    own, features = stream.shape
    lanes = rank // ROPE
    tail = rotary_key.reshape(lanes, length // lanes, ROPE).transpose(1, 0, 2)
    packed = jnp.concatenate([latent, tail.reshape(length // lanes, rank)], axis=0)
    half = ROPE // 2
    freqs = THETA ** (-jnp.arange(half, dtype=F32) / half)
    angle = jnp.arange(n * length, dtype=jnp.int32).astype(F32)[:, None] * freqs
    cosine, sine = jnp.cos(angle), jnp.sin(angle)
    table = jnp.concatenate([cosine, cosine, -sine, sine], axis=-1).reshape(n, length, 2 * ROPE)
    total = n * length
    heads_a = w_key_a.shape[1] // NOPE_A
    heads_b = w_key_b.shape[1] // NOPE_B
    width_a = -(-heads_a * V_A // 128) * 128
    width_b = heads_b * V_B
    hidden = w_up.shape[1] // 2
    V = pltpu.VMEM
    dma = lambda k: pltpu.SemaphoreType.DMA((k,))
    tokens = 2 * m * own
    scratch = [
        V((n,) + packed.shape, BF16),
        V((heads_a, total, NOPE_A + ROPE), BF16),
        V((heads_b, total, NOPE_B + ROPE), BF16),
        V((total, heads_a * V_A), BF16),
        V((total, heads_b * V_B), BF16),
        V((m, own, width_a + width_b), BF16),
        V((m, own, width_a + width_b), BF16),
        V((m - 1,) + w_out_a.shape, BF16),
        V((m - 1,) + w_out_b.shape, BF16),
        V((n, w_up.shape[0], hidden), BF16),
        V((n, hidden, w_down.shape[1]), BF16),
        V((tokens, features), BF16),
        V((tokens, hidden), F32),
        V((tokens, hidden), BF16),
        V((own, features), BF16),
        V((m, own, features), F32),
        V((m, own, features), BF16),
        V((m, own, features), BF16),
        V((own, features), BF16),
        V((2, own, features), BF16),
        V((3, own, features), BF16),
    ]
    sizes = [n, n, n, n, 3, 3, 3, 3, n, n, n, n, m, m, 8, 8, 4, 4]
    scratch += [dma(k) for k in sizes]
    return pl.pallas_call(
        functools.partial(kernel, n, m),
        out_shape=jax.ShapeDtypeStruct((own, features), BF16),
        in_specs=[pl.BlockSpec(memory_space=V)] * 17,
        out_specs=pl.BlockSpec(memory_space=V),
        scratch_shapes=scratch,
        compiler_params=pltpu.CompilerParams(
            collective_id=0, has_side_effects=True, vmem_limit_bytes=67043328),
        name="layer",
    )(stream, query_a, query_b, packed, table, latent_gain[None], key_gain_a[None],
      key_gain_b[None], w_key_a, w_value_a, w_key_b, w_value_b, w_out_a, w_out_b,
      norm_gain[None], w_up, w_down)


def solution(mesh):
    n, m = mesh.shape["sp"], mesh.shape["tp"]
    in_specs = (
        P(("sp", "tp"), None),
        P("sp", "tp"),
        P("sp", "tp"),
        P("sp", None),
        P("sp", None),
        P(),
        P(),
        P(),
        P(None, "tp"),
        P(None, "tp"),
        P(None, "tp"),
        P(None, "tp"),
        P("tp", None),
        P("tp", None),
        P(),
        P("sp", "tp"),
        P("tp", "sp"),
    )
    out_specs = P(("sp", "tp"), None)
    return jax.shard_map(functools.partial(body, n, m), mesh=mesh, in_specs=in_specs,
                         out_specs=out_specs, check_vma=False)
```

```python
import functools

import jax
import jax.numpy as jnp
import numpy as np
from jax import lax
from jax.experimental import pallas as pl
from jax.experimental.pallas import tpu as pltpu
from jax.sharding import PartitionSpec as P

NOPE_A = 64
V_A = 64
NOPE_B = 128
V_B = 128
ROPE = 32

EPSILON = 1e-06
THETA = 10000.0
F32 = jnp.float32
BF16 = jnp.bfloat16


def kernel(
    n, m,
    stream, q_a, q_b, packed, table, lat_gain, gain_a, gain_b,
    wk_a, wv_a, wk_b, wv_b, wo_a, wo_b, norm_gain, w_up, w_down,
    out,
    lat, key_a, key_b, val_a, val_b, att, rows, goa, gob,
    gup, gdown, x, hid, act, res, even, odd, sib, mid, part, land,
    lat_s, lat_r, latf_s, latf_r, oa_s, oa_r, ob_s, ob_r,
    up_s, up_r, dn_s, dn_r, at_s, at_r, x_s, x_r, rs_s, rs_r,
):
    s = lax.axis_index("sp")
    t = lax.axis_index("tp")
    core = t & 1
    length = q_a.shape[1]
    own = stream.shape[0]
    prow = packed.shape[0]
    half_rows = prow // 2
    depth_a = NOPE_A + ROPE
    depth_b = NOPE_B + ROPE
    heads_a = wk_a.shape[0] // NOPE_A
    heads_b = wk_b.shape[1] // NOPE_B
    hidden = gup.shape[2]
    wrows = w_up.shape[0]
    wcols = w_down.shape[1]
    width_a = heads_a * V_A
    width_b = heads_b * V_B
    start_b = att.shape[2] - width_b
    pending = []

    def copy(src, dst, ssem, rsem, sp, tp):
        return pltpu.make_async_remote_copy(
            src_ref=src, dst_ref=dst, send_sem=ssem, recv_sem=rsem,
            device_id={"sp": sp, "tp": tp}, device_id_type=pl.DeviceIdType.MESH,
        )

    def send(*args):
        c = copy(*args)
        c.start()
        pending.append(c)

    barrier = pltpu.get_barrier_semaphore()
    for k in range(1, n):
        pl.semaphore_signal(barrier, inc=1, device_id={"sp": s ^ k, "tp": t},
                            device_id_type=pl.DeviceIdType.MESH)
    for k in range(1, m):
        pl.semaphore_signal(barrier, inc=1, device_id={"sp": s, "tp": t ^ k},
                            device_id_type=pl.DeviceIdType.MESH)
    pl.semaphore_wait(barrier, n + m - 2)

    mine = pl.ds(pl.multiple_of(core * half_rows, 16), half_rows)
    other = pl.ds(pl.multiple_of((1 - core) * half_rows, 16), half_rows)
    for k in [1] + list(range(2, n, 2)):
        send(packed.at[mine], lat.at[k, mine], lat_s.at[k], lat_r.at[k], s ^ k, t)
    for k in (2, 1):
        send(wo_a, goa.at[k - 1], oa_s.at[k - 1], oa_r.at[k - 1], s, t ^ k)
        send(wo_b, gob.at[k - 1], ob_s.at[k - 1], ob_r.at[k - 1], s, t ^ k)

    def halves(target):
        return pl.ds(pl.multiple_of(((target // 2) % 2) * hidden, 128), hidden)

    for k in [1] + list(range(2, n, 2)):
        send(w_up.at[:, halves(s ^ k)], gup.at[k], up_s.at[k], up_r.at[k], s ^ k, t)
    for k in [1] + list(range(2, n, 2)):
        send(w_down.at[halves(s ^ k)], gdown.at[k], dn_s.at[k], dn_r.at[k], s ^ k, t)

    def make_block(k, source):
        start = pl.multiple_of(k * length, length)
        at = pl.ds(start, length)
        wide = source[0:length, :].astype(F32)
        normed = (wide * lax.rsqrt(jnp.mean(wide * wide, axis=-1, keepdims=True) + EPSILON)
                  * lat_gain[...]).astype(BF16)
        tail = source[length:prow, :].astype(F32)
        lanes = tail.shape[1] // ROPE
        rotary = jnp.concatenate([tail[:, i * ROPE:(i + 1) * ROPE] for i in range(lanes)], axis=0)
        squares = jnp.sum(rotary * rotary, axis=-1, keepdims=True)
        half = ROPE // 2
        turn = table[s ^ k]
        cosine = jnp.concatenate([turn[:, :half], turn[:, :half]], axis=-1)
        sine = jnp.concatenate([-turn[:, half:], turn[:, half:]], axis=-1)

        def turned(w):
            return lax.dot_general(normed, w[...], (((1,), (1,)), ((), ())),
                                   preferred_element_type=F32)

        def keys(flat, gain, nope, heads, dest):
            flat = flat.astype(BF16).astype(F32)
            for h in range(heads):
                piece = flat[:, h * nope:(h + 1) * nope]
                mean = (jnp.sum(piece * piece, axis=-1, keepdims=True) + squares) / (nope + ROPE)
                scale = lax.rsqrt(mean + EPSILON)
                dest[h, at, 0:nope] = (piece * scale * gain[:, 0:nope]).astype(BF16)
                last = rotary * scale * gain[:, nope:nope + ROPE]
                swapped = jnp.concatenate([last[:, half:], last[:, :half]], axis=-1)
                dest[h, at, nope:nope + ROPE] = (
                    last * cosine + swapped * sine).astype(BF16)

        keys(turned(wk_a), gain_a, NOPE_A, heads_a, key_a)
        keys(jnp.dot(normed, wk_b[...], preferred_element_type=F32), gain_b, NOPE_B, heads_b, key_b)
        val_a[at, :] = turned(wv_a).astype(BF16)
        val_b[at, :] = jnp.dot(normed, wv_b[...], preferred_element_type=F32).astype(BF16)

    make_block(0, packed)
    def arrived(k):
        copy(packed.at[mine], lat.at[k, mine], lat_s.at[k], lat_r.at[k], s ^ k, t).wait_recv()

    def to_sibling(k):
        send(lat.at[k, mine], lat.at[k, mine], latf_s.at[k], latf_r.at[k], s, t ^ 1)

    arrived(1)
    to_sibling(1)
    for k in range(2, n, 2):
        arrived(k)
        send(lat.at[k, mine], lat.at[k + 1, mine], lat_s.at[k + 1], lat_r.at[k + 1], s ^ 1, t)
        to_sibling(k)

    def weights_on(ref, ssem, rsem, k):
        copy(ref.at[k], ref.at[k], ssem.at[k], rsem.at[k], s ^ k, t).wait_recv()
        send(ref.at[k], ref.at[k + 1], ssem.at[k + 1], rsem.at[k + 1], s ^ 1, t)

    for k in range(3, n, 2):
        arrived(k)
        to_sibling(k)

    def one(k, carry):
        copy(lat.at[k, other], lat.at[k, other], latf_s.at[k], latf_r.at[k], s, t ^ 1).wait_recv()
        make_block(k, lat.at[k])
        return carry

    lax.fori_loop(1, n, one, 0)
    weights_on(gup, up_s, up_r, 2)

    total = n * length
    block = min(total, 2048)
    number = total // block

    def attend(q, key, value, h, depth, width):
        query = q[h * depth:(h + 1) * depth, :].T

        def step(i, state):
            peak, sums, acc = state
            at = pl.ds(pl.multiple_of(i * block, block), block)
            score = lax.dot_general(query, key[h, at, :], (((1,), (1,)), ((), ())),
                                    preferred_element_type=F32) * depth ** (-0.5)
            new = jnp.maximum(peak, jnp.max(score, axis=-1, keepdims=True))
            shifted = jnp.exp(score - new)
            factor = jnp.exp(peak - new)
            sums = sums * factor + jnp.sum(shifted, axis=-1, keepdims=True)
            acc = acc * factor + jnp.dot(
                shifted.astype(BF16), value[at, h * width:(h + 1) * width],
                preferred_element_type=F32)
            return new, sums, acc

        state = (jnp.full((length, 1), -jnp.inf, F32), jnp.zeros((length, 1), F32),
                 jnp.zeros((length, width), F32))
        if number == 1:
            state = step(0, state)
        else:
            state = lax.fori_loop(0, number, step, state)
        return (state[2] / state[1]).astype(BF16)

    for h in range(heads_a):
        res_a = attend(q_a, key_a, val_a, h, depth_a, V_A)
        for j in range(m):
            att[j, :, h * V_A:(h + 1) * V_A] = res_a[j * own:(j + 1) * own]
    weights_on(gup, up_s, up_r, 4)
    copy(wo_a, goa.at[1], oa_s.at[1], oa_r.at[1], s, t ^ 2).wait_recv()
    send(goa.at[1], goa.at[2], oa_s.at[2], oa_r.at[2], s, t ^ 1)
    copy(wo_b, gob.at[1], ob_s.at[1], ob_r.at[1], s, t ^ 2).wait_recv()
    send(gob.at[1], gob.at[2], ob_s.at[2], ob_r.at[2], s, t ^ 1)
    for h in range(heads_b):
        res_b = attend(q_b, key_b, val_b, h, depth_b, V_B)
        for j in range(m):
            att[j, :, start_b + h * V_B:start_b + (h + 1) * V_B] = res_b[j * own:(j + 1) * own]
    for k in range(1, m):
        send(att.at[t ^ k], rows.at[k], at_s.at[k], at_r.at[k], s, t ^ k)

    mixed = (jnp.dot(att[t, :, 0:width_a], wo_a[...], preferred_element_type=F32)
             + jnp.dot(att[t, :, start_b:], wo_b[...], preferred_element_type=F32))
    for k in range(1, m):
        copy(wo_a, goa.at[k - 1], oa_s.at[k - 1], oa_r.at[k - 1], s, t ^ 1) \
            .wait_recv() if k != 2 else None
        copy(wo_b, gob.at[k - 1], ob_s.at[k - 1], ob_r.at[k - 1], s, t ^ 1) \
            .wait_recv() if k != 2 else None
        copy(att.at[t ^ k], rows.at[k], at_s.at[k], at_r.at[k], s, t ^ k).wait_recv()
        mixed += jnp.dot(rows[k, :, 0:width_a], goa[k - 1], preferred_element_type=F32)
        mixed += jnp.dot(rows[k, :, start_b:], gob[k - 1], preferred_element_type=F32)
    residual = (stream[...].astype(F32) + mixed).astype(BF16)
    res[...] = residual
    wide = residual.astype(F32)
    x[0:own, :] = (wide * lax.rsqrt(jnp.mean(wide * wide, axis=-1, keepdims=True) + EPSILON)
                   * norm_gain[...]).astype(BF16)

    def peer(code):
        return (s ^ 2 if code & 4 else s), t ^ (code & 3)

    def slot(k):
        return x.at[pl.ds(k * own, own)]

    def xcopy(src, dst, code):
        return copy(slot(src), slot(dst), x_s.at[dst], x_r.at[dst], *peer(code))

    def xsend(src, dst, code):
        c = xcopy(src, dst, code)
        c.start()
        pending.append(c)

    for code in (2, 4, 1):
        xsend(0, code, code)
    for k in range(6, n, 2):
        weights_on(gup, up_s, up_r, k)
    xcopy(0, 2, 2).wait_recv()
    xcopy(0, 4, 4).wait_recv()
    diag = copy(
        x.at[pl.ds(pl.multiple_of((2 + 2 * core) * own, own), own)], slot(6),
        x_s.at[6], x_r.at[6], s ^ (2 - 2 * core), t ^ (2 * core))
    diag.start()
    pending.append(diag)
    xsend(2, 3, 1)
    xsend(4, 5, 1)
    diag.wait_recv()
    xsend(6, 7, 1)
    weights_on(gdown, dn_s, dn_r, 2)
    for k in (1, 3, 5, 7):
        xcopy(k - 1, k, 1).wait_recv()

    def columns(k, size):
        return pl.ds(pl.multiple_of((s ^ k) * size, 128), size)

    held = halves(s)
    hid[...] = jnp.dot(x[:, columns(0, wrows)], w_up[:, held], preferred_element_type=F32)

    def up(k):
        hid[...] += jnp.dot(x[:, columns(k, wrows)], gup[k], preferred_element_type=F32)

    def up_loop(i, carry):
        k = 2 * i
        copy(gup.at[k + 1], gup.at[k + 1], up_s.at[k + 1], up_r.at[k + 1], s ^ 1, t).wait_recv()
        up(k)
        up(k + 1)
        return carry

    copy(gup.at[1], gup.at[1], up_s.at[1], up_r.at[1], s ^ 1, t).wait_recv()
    up(1)
    lax.fori_loop(1, 3, up_loop, 0)
    weights_on(gdown, dn_s, dn_r, 4)
    lax.fori_loop(3, n // 2, up_loop, 0)
    act[...] = jnp.square(jnp.maximum(hid[...], 0.0)).astype(BF16)

    group = n // 2

    def split(g, k, piece):
        at = pl.ds(pl.multiple_of(((s ^ k) % group) * wcols, 128), wcols)
        for i in range(4):
            even[g, i, :, at] = piece[2 * i * own:(2 * i + 1) * own]
            odd[g, i, :, at] = piece[(2 * i + 1) * own:(2 * i + 2) * own].astype(BF16)

    def down(g, k):
        split(g, k, jnp.dot(act[...], gdown[k], preferred_element_type=F32))

    def down_loop(g):
        def step(i, carry):
            k = 2 * i
            down(g, k)
            copy(gdown.at[k + 1], gdown.at[k + 1], dn_s.at[k + 1], dn_r.at[k + 1],
                 s ^ 1, t).wait_recv()
            down(g, k + 1)
            return carry
        return step

    def first(g):
        return copy(odd.at[g], sib.at[g], rs_s.at[4 * g], rs_r.at[4 * g], s, t ^ 1)

    def second(g):
        return copy(mid.at[g], land.at[g, 0], rs_s.at[4 * g + 1], rs_r.at[4 * g + 1],
                    s ^ (2 - 2 * core), t ^ (2 * core))

    def third(g):
        return copy(part.at[g, 0], land.at[g, 1], rs_s.at[4 * g + 2], rs_r.at[4 * g + 2],
                    s, t ^ 2)

    def fourth(g):
        return copy(part.at[g, 1], land.at[g, 2], rs_s.at[4 * g + 3], rs_r.at[4 * g + 3],
                    s ^ 2, t)

    def begin(c):
        c.start()
        pending.append(c)

    def diagonal(g):
        first(g).wait_recv()
        mid[g] = (even[g, 3] + sib[g, 3].astype(F32)).astype(BF16)
        begin(second(g))
        for i in range(3):
            even[g, i] += sib[g, i].astype(F32)

    def straight(g):
        second(g).wait_recv()
        even[g, 1 + core] += land[g, 0].astype(F32)
        for i in (1, 2):
            part[g, i - 1] = even[g, i].astype(BF16)
        begin(third(g))
        begin(fourth(g))

    def finish(g):
        third(g).wait_recv()
        fourth(g).wait_recv()
        summed = even[g, 0] + land[g, 1].astype(F32) + land[g, 2].astype(F32)
        base = (s // group) if g == 0 else 1 - s // group
        at = pl.ds(pl.multiple_of(base * (group * wcols), 128), group * wcols)
        out[:, at] = (res[:, at].astype(F32) + summed).astype(BF16)

    split(0, 0, jnp.dot(act[...], w_down[held, :], preferred_element_type=F32))
    copy(gdown.at[1], gdown.at[1], dn_s.at[1], dn_r.at[1], s ^ 1, t).wait_recv()
    down(0, 1)
    for k in range(6, n, 2):
        weights_on(gdown, dn_s, dn_r, k)
    lax.fori_loop(1, group // 2, down_loop(0), 0)
    begin(first(0))
    diagonal(0)
    lax.fori_loop(group // 2, n // 2, down_loop(1), 0)
    straight(0)
    begin(first(1))
    diagonal(1)
    finish(0)
    straight(1)
    finish(1)
    for c in pending:
        c.wait_send()


def body(n, m, stream, query_a, query_b, latent, rotary_key, latent_gain, key_gain_a, key_gain_b,
         w_key_a, w_value_a, w_key_b, w_value_b, w_out_a, w_out_b, norm_gain, w_up, w_down):
    length, rank = latent.shape
    own, features = stream.shape
    lanes = rank // ROPE
    tail = rotary_key.reshape(lanes, length // lanes, ROPE).transpose(1, 0, 2)
    packed = jnp.concatenate([latent, tail.reshape(length // lanes, rank)], axis=0)
    half = ROPE // 2
    freqs = np.float32(THETA) ** (-np.arange(half, dtype=np.float32) / np.float32(half))
    angle = np.arange(n * length).astype(np.float32)[:, None] * freqs
    cosine, sine = np.cos(angle), np.sin(angle)
    table = jnp.asarray(np.concatenate([cosine, sine], axis=-1).reshape(n, length, ROPE))
    total = n * length
    heads_a = w_key_a.shape[1] // NOPE_A
    heads_b = w_key_b.shape[1] // NOPE_B
    width_a = -(-heads_a * V_A // 128) * 128
    width_b = heads_b * V_B
    hidden = w_up.shape[1] // 2
    V = pltpu.VMEM
    dma = lambda k: pltpu.SemaphoreType.DMA((k,))
    tokens = 2 * m * own
    scratch = [
        V((n,) + packed.shape, BF16),
        V((heads_a, total, NOPE_A + ROPE), BF16),
        V((heads_b, total, NOPE_B + ROPE), BF16),
        V((total, heads_a * V_A), BF16),
        V((total, heads_b * V_B), BF16),
        V((m, own, width_a + width_b), BF16),
        V((m, own, width_a + width_b), BF16),
        V((m - 1,) + w_out_a.shape, BF16),
        V((m - 1,) + w_out_b.shape, BF16),
        V((n, w_up.shape[0], hidden), BF16),
        V((n, hidden, w_down.shape[1]), BF16),
        V((tokens, features), BF16),
        V((tokens, hidden), F32),
        V((tokens, hidden), BF16),
        V((own, features), BF16),
        V((2, 4, own, features // 2), F32),
        V((2, 4, own, features // 2), BF16),
        V((2, 4, own, features // 2), BF16),
        V((2, own, features // 2), BF16),
        V((2, 2, own, features // 2), BF16),
        V((2, 3, own, features // 2), BF16),
    ]
    sizes = [n, n, n, n, 3, 3, 3, 3, n, n, n, n, m, m, 8, 8, 8, 8]
    scratch += [dma(k) for k in sizes]
    return pl.pallas_call(
        functools.partial(kernel, n, m),
        out_shape=jax.ShapeDtypeStruct((own, features), BF16),
        in_specs=[pl.BlockSpec(memory_space=V)] * 17,
        out_specs=pl.BlockSpec(memory_space=V),
        scratch_shapes=scratch,
        compiler_params=pltpu.CompilerParams(
            collective_id=0, has_side_effects=True, vmem_limit_bytes=67043328),
        name="layer",
    )(stream, query_a.T, query_b.T, packed, table, latent_gain[None], key_gain_a[None],
      key_gain_b[None], w_key_a.T, w_value_a.T, w_key_b, w_value_b, w_out_a, w_out_b,
      norm_gain[None], w_up, w_down)


def solution(mesh):
    n, m = mesh.shape["sp"], mesh.shape["tp"]
    in_specs = (
        P(("sp", "tp"), None),
        P("sp", "tp"),
        P("sp", "tp"),
        P("sp", None),
        P("sp", None),
        P(),
        P(),
        P(),
        P(None, "tp"),
        P(None, "tp"),
        P(None, "tp"),
        P(None, "tp"),
        P("tp", None),
        P("tp", None),
        P(),
        P("sp", "tp"),
        P("tp", "sp"),
    )
    out_specs = P(("sp", "tp"), None)
    return jax.shard_map(functools.partial(body, n, m), mesh=mesh, in_specs=in_specs,
                         out_specs=out_specs, check_vma=False)
```

```python
import functools

import jax
import jax.numpy as jnp
import numpy as np
from jax import lax
from jax.experimental import pallas as pl
from jax.experimental.pallas import tpu as pltpu
from jax.sharding import PartitionSpec as P

NOPE_A = 64
V_A = 64
NOPE_B = 128
V_B = 128
ROPE = 32

EPSILON = 1e-06
THETA = 10000.0
F32 = jnp.float32
BF16 = jnp.bfloat16


def kernel(
    n, m,
    stream, q_a, q_b, packed, table, lat_gain, gain_a, gain_b,
    wk_a, wv_a, wk_b, wv_b, wo_a, wo_b, norm_gain, w_up, w_down,
    out,
    lat, key_a, key_b, val_a, val_b, att, rows, goa, gob,
    gup, gdown, x, hid, act, res, even, odd, sib, mid, part, land,
    lat_s, lat_r, latf_s, latf_r, oa_s, oa_r, ob_s, ob_r,
    up_s, up_r, dn_s, dn_r, at_s, at_r, x_s, x_r, rs_s, rs_r,
):
    s = lax.axis_index("sp")
    t = lax.axis_index("tp")
    core = t & 1
    length = q_a.shape[1]
    own = stream.shape[0]
    prow = packed.shape[0]
    half_rows = prow // 2
    depth_a = NOPE_A + ROPE
    depth_b = NOPE_B + ROPE
    heads_a = wk_a.shape[0] // NOPE_A
    heads_b = wk_b.shape[1] // NOPE_B
    hidden = gup.shape[2]
    wrows = w_up.shape[0]
    wcols = w_down.shape[1]
    width_a = heads_a * V_A
    width_b = heads_b * V_B
    start_b = att.shape[2] - width_b
    pending = []

    def copy(src, dst, ssem, rsem, sp, tp):
        return pltpu.make_async_remote_copy(
            src_ref=src, dst_ref=dst, send_sem=ssem, recv_sem=rsem,
            device_id={"sp": sp, "tp": tp}, device_id_type=pl.DeviceIdType.MESH,
        )

    def send(*args):
        c = copy(*args)
        c.start()
        pending.append(c)

    barrier = pltpu.get_barrier_semaphore()
    for k in range(1, n):
        pl.semaphore_signal(barrier, inc=1, device_id={"sp": s ^ k, "tp": t},
                            device_id_type=pl.DeviceIdType.MESH)
    for k in range(1, m):
        pl.semaphore_signal(barrier, inc=1, device_id={"sp": s, "tp": t ^ k},
                            device_id_type=pl.DeviceIdType.MESH)
    pl.semaphore_wait(barrier, n + m - 2)

    mine = pl.ds(pl.multiple_of(core * half_rows, 16), half_rows)
    other = pl.ds(pl.multiple_of((1 - core) * half_rows, 16), half_rows)
    for k in [1] + list(range(2, n, 2)):
        send(packed.at[mine], lat.at[k, mine], lat_s.at[k], lat_r.at[k], s ^ k, t)
    for k in (2, 1):
        send(wo_a, goa.at[k - 1], oa_s.at[k - 1], oa_r.at[k - 1], s, t ^ k)
        send(wo_b, gob.at[k - 1], ob_s.at[k - 1], ob_r.at[k - 1], s, t ^ k)

    def halves(target):
        return pl.ds(pl.multiple_of(((target // 2) % 2) * hidden, 128), hidden)

    for k in [1] + list(range(2, n, 2)):
        send(w_up.at[:, halves(s ^ k)], gup.at[k], up_s.at[k], up_r.at[k], s ^ k, t)
    for k in [1] + list(range(2, n, 2)):
        send(w_down.at[halves(s ^ k)], gdown.at[k], dn_s.at[k], dn_r.at[k], s ^ k, t)

    def make_block(k, source):
        start = pl.multiple_of(k * length, length)
        at = pl.ds(start, length)
        wide = source[0:length, :].astype(F32)
        normed = (wide * lax.rsqrt(jnp.mean(wide * wide, axis=-1, keepdims=True) + EPSILON)
                  * lat_gain[...]).astype(BF16)
        tail = source[length:prow, :].astype(F32)
        lanes = tail.shape[1] // ROPE
        rotary = jnp.concatenate([tail[:, i * ROPE:(i + 1) * ROPE] for i in range(lanes)], axis=0)
        squares = jnp.sum(rotary * rotary, axis=-1, keepdims=True)
        half = ROPE // 2
        turn = table[s ^ k]
        cosine = jnp.concatenate([turn[:, :half], turn[:, :half]], axis=-1)
        sine = jnp.concatenate([-turn[:, half:], turn[:, half:]], axis=-1)

        def turned(w):
            return lax.dot_general(normed, w[...], (((1,), (1,)), ((), ())),
                                   preferred_element_type=F32)

        def keys(flat, gain, nope, heads, dest):
            flat = flat.astype(BF16).astype(F32)
            for h in range(heads):
                piece = flat[:, h * nope:(h + 1) * nope]
                mean = (jnp.sum(piece * piece, axis=-1, keepdims=True) + squares) / (nope + ROPE)
                scale = lax.rsqrt(mean + EPSILON)
                dest[h, at, 0:nope] = (piece * scale * gain[:, 0:nope]).astype(BF16)
                last = rotary * scale * gain[:, nope:nope + ROPE]
                swapped = jnp.concatenate([last[:, half:], last[:, :half]], axis=-1)
                dest[h, at, nope:nope + ROPE] = (
                    last * cosine + swapped * sine).astype(BF16)

        keys(turned(wk_a), gain_a, NOPE_A, heads_a, key_a)
        keys(jnp.dot(normed, wk_b[...], preferred_element_type=F32), gain_b, NOPE_B, heads_b, key_b)
        val_a[at, :] = turned(wv_a).astype(BF16)
        val_b[at, :] = jnp.dot(normed, wv_b[...], preferred_element_type=F32).astype(BF16)

    make_block(0, packed)
    def arrived(k):
        copy(packed.at[mine], lat.at[k, mine], lat_s.at[k], lat_r.at[k], s ^ k, t).wait_recv()

    def to_sibling(k):
        send(lat.at[k, mine], lat.at[k, mine], latf_s.at[k], latf_r.at[k], s, t ^ 1)

    arrived(1)
    to_sibling(1)
    for k in range(2, n, 2):
        arrived(k)
        send(lat.at[k, mine], lat.at[k + 1, mine], lat_s.at[k + 1], lat_r.at[k + 1], s ^ 1, t)
        to_sibling(k)

    def weights_on(ref, ssem, rsem, k):
        copy(ref.at[k], ref.at[k], ssem.at[k], rsem.at[k], s ^ k, t).wait_recv()
        send(ref.at[k], ref.at[k + 1], ssem.at[k + 1], rsem.at[k + 1], s ^ 1, t)

    for k in range(3, n, 2):
        arrived(k)
        to_sibling(k)

    def one(k, carry):
        copy(lat.at[k, other], lat.at[k, other], latf_s.at[k], latf_r.at[k], s, t ^ 1).wait_recv()
        make_block(k, lat.at[k])
        return carry

    lax.fori_loop(1, n, one, 0)
    weights_on(gup, up_s, up_r, 2)
    weights_on(gup, up_s, up_r, 4)

    total = n * length
    block = min(total, 2048)
    number = total // block

    def attend(q, key, value, h, depth, width):
        query = q[h * depth:(h + 1) * depth, :].T

        def step(i, state):
            peak, sums, acc = state
            at = pl.ds(pl.multiple_of(i * block, block), block)
            score = lax.dot_general(query, key[h, at, :], (((1,), (1,)), ((), ())),
                                    preferred_element_type=F32) * depth ** (-0.5)
            new = jnp.maximum(peak, jnp.max(score, axis=-1, keepdims=True))
            shifted = jnp.exp(score - new)
            factor = jnp.exp(peak - new)
            sums = sums * factor + jnp.sum(shifted, axis=-1, keepdims=True)
            acc = acc * factor + jnp.dot(
                shifted.astype(BF16), value[at, h * width:(h + 1) * width],
                preferred_element_type=F32)
            return new, sums, acc

        state = (jnp.full((length, 1), -jnp.inf, F32), jnp.zeros((length, 1), F32),
                 jnp.zeros((length, width), F32))
        if number == 1:
            state = step(0, state)
        else:
            state = lax.fori_loop(0, number, step, state)
        return (state[2] / state[1]).astype(BF16)

    for h in range(heads_a):
        res_a = attend(q_a, key_a, val_a, h, depth_a, V_A)
        for j in range(m):
            att[j, :, h * V_A:(h + 1) * V_A] = res_a[j * own:(j + 1) * own]
    copy(wo_a, goa.at[1], oa_s.at[1], oa_r.at[1], s, t ^ 2).wait_recv()
    send(goa.at[1], goa.at[2], oa_s.at[2], oa_r.at[2], s, t ^ 1)
    copy(wo_b, gob.at[1], ob_s.at[1], ob_r.at[1], s, t ^ 2).wait_recv()
    send(gob.at[1], gob.at[2], ob_s.at[2], ob_r.at[2], s, t ^ 1)
    for h in range(heads_b):
        res_b = attend(q_b, key_b, val_b, h, depth_b, V_B)
        for j in range(m):
            att[j, :, start_b + h * V_B:start_b + (h + 1) * V_B] = res_b[j * own:(j + 1) * own]
    for k in range(1, m):
        send(att.at[t ^ k], rows.at[k], at_s.at[k], at_r.at[k], s, t ^ k)

    mixed = (jnp.dot(att[t, :, 0:width_a], wo_a[...], preferred_element_type=F32)
             + jnp.dot(att[t, :, start_b:], wo_b[...], preferred_element_type=F32))
    for k in range(1, m):
        copy(wo_a, goa.at[k - 1], oa_s.at[k - 1], oa_r.at[k - 1], s, t ^ 1) \
            .wait_recv() if k != 2 else None
        copy(wo_b, gob.at[k - 1], ob_s.at[k - 1], ob_r.at[k - 1], s, t ^ 1) \
            .wait_recv() if k != 2 else None
        copy(att.at[t ^ k], rows.at[k], at_s.at[k], at_r.at[k], s, t ^ k).wait_recv()
        mixed += jnp.dot(rows[k, :, 0:width_a], goa[k - 1], preferred_element_type=F32)
        mixed += jnp.dot(rows[k, :, start_b:], gob[k - 1], preferred_element_type=F32)
    residual = (stream[...].astype(F32) + mixed).astype(BF16)
    res[...] = residual
    wide = residual.astype(F32)
    x[0:own, :] = (wide * lax.rsqrt(jnp.mean(wide * wide, axis=-1, keepdims=True) + EPSILON)
                   * norm_gain[...]).astype(BF16)

    def peer(code):
        return (s ^ 2 if code & 4 else s), t ^ (code & 3)

    def slot(k):
        return x.at[pl.ds(k * own, own)]

    def xcopy(src, dst, code):
        return copy(slot(src), slot(dst), x_s.at[dst], x_r.at[dst], *peer(code))

    def xsend(src, dst, code):
        c = xcopy(src, dst, code)
        c.start()
        pending.append(c)

    for code in (2, 4, 1):
        xsend(0, code, code)
    for k in range(6, n, 2):
        weights_on(gup, up_s, up_r, k)
    weights_on(gdown, dn_s, dn_r, 2)
    xcopy(0, 2, 2).wait_recv()
    xcopy(0, 4, 4).wait_recv()
    diag = copy(
        x.at[pl.ds(pl.multiple_of((2 + 2 * core) * own, own), own)], slot(6),
        x_s.at[6], x_r.at[6], s ^ (2 - 2 * core), t ^ (2 * core))
    diag.start()
    pending.append(diag)
    xsend(2, 3, 1)
    xsend(4, 5, 1)
    diag.wait_recv()
    xsend(6, 7, 1)
    weights_on(gdown, dn_s, dn_r, 4)
    for k in (1, 3, 5, 7):
        xcopy(k - 1, k, 1).wait_recv()

    def columns(k, size):
        return pl.ds(pl.multiple_of((s ^ k) * size, 128), size)

    held = halves(s)
    hid[...] = jnp.dot(x[:, columns(0, wrows)], w_up[:, held], preferred_element_type=F32)

    def up(k):
        hid[...] += jnp.dot(x[:, columns(k, wrows)], gup[k], preferred_element_type=F32)

    def up_loop(i, carry):
        k = 2 * i
        copy(gup.at[k + 1], gup.at[k + 1], up_s.at[k + 1], up_r.at[k + 1], s ^ 1, t).wait_recv()
        up(k)
        up(k + 1)
        return carry

    copy(gup.at[1], gup.at[1], up_s.at[1], up_r.at[1], s ^ 1, t).wait_recv()
    up(1)
    lax.fori_loop(1, 3, up_loop, 0)
    lax.fori_loop(3, n // 2, up_loop, 0)
    for k in range(6, n, 2):
        weights_on(gdown, dn_s, dn_r, k)
    act[...] = jnp.square(jnp.maximum(hid[...], 0.0)).astype(BF16)

    group = n // 2

    def split(g, k, piece):
        at = pl.ds(pl.multiple_of(((s ^ k) % group) * wcols, 128), wcols)
        for i in range(4):
            even[g, i, :, at] = piece[2 * i * own:(2 * i + 1) * own]
            odd[g, i, :, at] = piece[(2 * i + 1) * own:(2 * i + 2) * own].astype(BF16)

    def down(g, k):
        split(g, k, jnp.dot(act[...], gdown[k], preferred_element_type=F32))

    def down_loop(g):
        def step(i, carry):
            k = 2 * i
            down(g, k)
            copy(gdown.at[k + 1], gdown.at[k + 1], dn_s.at[k + 1], dn_r.at[k + 1],
                 s ^ 1, t).wait_recv()
            down(g, k + 1)
            return carry
        return step

    def first(g):
        return copy(odd.at[g], sib.at[g], rs_s.at[4 * g], rs_r.at[4 * g], s, t ^ 1)

    def second(g):
        return copy(mid.at[g], land.at[g, 0], rs_s.at[4 * g + 1], rs_r.at[4 * g + 1],
                    s ^ (2 - 2 * core), t ^ (2 * core))

    def third(g):
        return copy(part.at[g, 0], land.at[g, 1], rs_s.at[4 * g + 2], rs_r.at[4 * g + 2],
                    s, t ^ 2)

    def fourth(g):
        return copy(part.at[g, 1], land.at[g, 2], rs_s.at[4 * g + 3], rs_r.at[4 * g + 3],
                    s ^ 2, t)

    def begin(c):
        c.start()
        pending.append(c)

    def diagonal(g):
        first(g).wait_recv()
        mid[g] = (even[g, 3] + sib[g, 3].astype(F32)).astype(BF16)
        begin(second(g))
        for i in range(3):
            even[g, i] += sib[g, i].astype(F32)

    def straight(g):
        second(g).wait_recv()
        even[g, 1 + core] += land[g, 0].astype(F32)
        for i in (1, 2):
            part[g, i - 1] = even[g, i].astype(BF16)
        begin(third(g))
        begin(fourth(g))

    def finish(g):
        third(g).wait_recv()
        fourth(g).wait_recv()
        summed = even[g, 0] + land[g, 1].astype(F32) + land[g, 2].astype(F32)
        base = (s // group) if g == 0 else 1 - s // group
        at = pl.ds(pl.multiple_of(base * (group * wcols), 128), group * wcols)
        out[:, at] = (res[:, at].astype(F32) + summed).astype(BF16)

    split(0, 0, jnp.dot(act[...], w_down[held, :], preferred_element_type=F32))
    copy(gdown.at[1], gdown.at[1], dn_s.at[1], dn_r.at[1], s ^ 1, t).wait_recv()
    down(0, 1)
    lax.fori_loop(1, group // 2, down_loop(0), 0)
    begin(first(0))
    diagonal(0)
    lax.fori_loop(group // 2, n // 2, down_loop(1), 0)
    straight(0)
    begin(first(1))
    diagonal(1)
    finish(0)
    straight(1)
    finish(1)
    for c in pending:
        c.wait_send()


def body(n, m, stream, query_a, query_b, latent, rotary_key, latent_gain, key_gain_a, key_gain_b,
         w_key_a, w_value_a, w_key_b, w_value_b, w_out_a, w_out_b, norm_gain, w_up, w_down):
    length, rank = latent.shape
    own, features = stream.shape
    lanes = rank // ROPE
    tail = rotary_key.reshape(lanes, length // lanes, ROPE).transpose(1, 0, 2)
    packed = jnp.concatenate([latent, tail.reshape(length // lanes, rank)], axis=0)
    half = ROPE // 2
    freqs = np.float32(THETA) ** (-np.arange(half, dtype=np.float32) / np.float32(half))
    angle = np.arange(n * length).astype(np.float32)[:, None] * freqs
    cosine, sine = np.cos(angle), np.sin(angle)
    table = jnp.asarray(np.concatenate([cosine, sine], axis=-1).reshape(n, length, ROPE))
    total = n * length
    heads_a = w_key_a.shape[1] // NOPE_A
    heads_b = w_key_b.shape[1] // NOPE_B
    width_a = -(-heads_a * V_A // 128) * 128
    width_b = heads_b * V_B
    hidden = w_up.shape[1] // 2
    V = pltpu.VMEM
    dma = lambda k: pltpu.SemaphoreType.DMA((k,))
    tokens = 2 * m * own
    scratch = [
        V((n,) + packed.shape, BF16),
        V((heads_a, total, NOPE_A + ROPE), BF16),
        V((heads_b, total, NOPE_B + ROPE), BF16),
        V((total, heads_a * V_A), BF16),
        V((total, heads_b * V_B), BF16),
        V((m, own, width_a + width_b), BF16),
        V((m, own, width_a + width_b), BF16),
        V((m - 1,) + w_out_a.shape, BF16),
        V((m - 1,) + w_out_b.shape, BF16),
        V((n, w_up.shape[0], hidden), BF16),
        V((n, hidden, w_down.shape[1]), BF16),
        V((tokens, features), BF16),
        V((tokens, hidden), F32),
        V((tokens, hidden), BF16),
        V((own, features), BF16),
        V((2, 4, own, features // 2), F32),
        V((2, 4, own, features // 2), BF16),
        V((2, 4, own, features // 2), BF16),
        V((2, own, features // 2), BF16),
        V((2, 2, own, features // 2), BF16),
        V((2, 3, own, features // 2), BF16),
    ]
    sizes = [n, n, n, n, 3, 3, 3, 3, n, n, n, n, m, m, 8, 8, 8, 8]
    scratch += [dma(k) for k in sizes]
    return pl.pallas_call(
        functools.partial(kernel, n, m),
        out_shape=jax.ShapeDtypeStruct((own, features), BF16),
        in_specs=[pl.BlockSpec(memory_space=V)] * 17,
        out_specs=pl.BlockSpec(memory_space=V),
        scratch_shapes=scratch,
        compiler_params=pltpu.CompilerParams(
            collective_id=0, has_side_effects=True, vmem_limit_bytes=67043328),
        name="layer",
    )(stream, query_a.T, query_b.T, packed, table, latent_gain[None], key_gain_a[None],
      key_gain_b[None], w_key_a.T, w_value_a.T, w_key_b, w_value_b, w_out_a, w_out_b,
      norm_gain[None], w_up, w_down)


def solution(mesh):
    n, m = mesh.shape["sp"], mesh.shape["tp"]
    in_specs = (
        P(("sp", "tp"), None),
        P("sp", "tp"),
        P("sp", "tp"),
        P("sp", None),
        P("sp", None),
        P(),
        P(),
        P(),
        P(None, "tp"),
        P(None, "tp"),
        P(None, "tp"),
        P(None, "tp"),
        P("tp", None),
        P("tp", None),
        P(),
        P("sp", "tp"),
        P("tp", "sp"),
    )
    out_specs = P(("sp", "tp"), None)
    return jax.shard_map(functools.partial(body, n, m), mesh=mesh, in_specs=in_specs,
                         out_specs=out_specs, check_vma=False)
```
